32 devices in a mesh: grp: 2 (over y), fs: 4 (over z), tp: 4 (over x, core).
Axes of the slice: x: 2, y: 2, z: 4, core: 2. Of those that a mesh axis runs over, the one named last changes fastest.
Arguments:
- tokens: bfloat16 [4096, 2048], P(('grp', 'fs', 'tp')), parts along dimension 0, may hold values from -12 to 12
- norm_gain: float32 [2048], replicated, may hold values from 0.1 to 1.9
- w_in: bfloat16 [2048, 8192], P('fs', 'tp'), may hold values from -0.125 to 0.125
- w_out: bfloat16 [8192, 2048], P('tp', 'fs'), may hold values from -0.0625 to 0.0625
Outputs:
- mixed: bfloat16 [4096, 2048], P(('grp', 'fs', 'tp')), parts along dimension 0
The draws below stay inside these ranges and needn't reach their ends.
There are 2 independent parts, one for each index of `grp`. The reference program is written for one: setup_inputs(seed, part) draws one part's arguments, and reference() takes and returns one part's arrays. A program takes and returns all parts, laid end to end along the dimension named above; an argument that names none is the same for every part. Nothing has to cross between parts.
All inputs are finite; a program needn't handle non-finite values.
Results may differ from the reference program's by a relative error of at most 0.012.
Values may be sent and summed in bfloat16 or wider, within the bound.
A program may use at most 64 MiB of HBM per device.

```python
import math
import jax
import jax.numpy as jnp
from jax import lax

D = 2048
FF = 8192
FF_DEV = 2048
TOKENS = 2048
N_TP = 4


def draw_tokens(key, part):
    first = jax.random.fold_in(key, 11)
    second = jax.random.fold_in(key, 12)
    scales = jnp.exp(jax.random.uniform(second, (TOKENS, 1), jnp.float32, math.log(0.35), math.log(2.8)))
    base = jax.random.normal(first, (TOKENS, D), jnp.float32)
    return jnp.clip(base * scales, -12.0, 12.0).astype(jnp.bfloat16)


def block_scale(stream_key, extent, cuts, low, top_value):
    gain, own = 1.0, jax.random.fold_in(stream_key, 6)
    for position, shards_of in cuts:
        steps = jnp.exp(jax.random.uniform(jax.random.fold_in(own, position), (shards_of,), jnp.float32, low / len(cuts), top_value / len(cuts)))
        gain = gain * jnp.repeat(steps, extent[position] // shards_of).reshape([-1 if axis == position else 1 for axis in range(len(extent))])
    return gain


def gaussian(rng, dims, spread, bound, cuts=(), dtype=jnp.bfloat16):
    entries = jax.random.normal(rng, dims, jnp.float32) * spread
    if len(cuts) > 0:
        entries = block_scale(rng, dims, cuts, -0.22, 0.18) * entries
    return jnp.clip(entries, min=-bound, max=bound).astype(dtype)


def setup_inputs(seed: int = 0, part: int = 0) -> dict:
    key_list = jax.random.split(jax.random.key(seed), 5)
    own_keys = jax.random.split(jax.random.fold_in(key_list[4], part), 5)
    tokens = draw_tokens(jax.random.fold_in(jax.random.fold_in(key_list[4], part), 71), part)
    norm_gain = jnp.clip(1.0 + 0.18 * jax.random.normal(key_list[1], (D,), jnp.float32), 0.1, 1.9)
    w_in = gaussian(key_list[2], (D, FF), D ** -0.5, 0.125, ((0, 4), (1, 4)))
    w_out = gaussian(key_list[3], (FF, D), FF ** -0.5, 0.0625, ((0, 4), (1, 4)))
    return dict(tokens=tokens, norm_gain=norm_gain, w_in=w_in, w_out=w_out)


EPS = 1e-06

def reference(tokens, norm_gain, w_in, w_out):
    block = math.gcd(TOKENS, 2048)
    pieces = tokens.reshape(TOKENS // block, block, D)

    def one_block(rows_in):
        xf = rows_in.astype(jnp.float32)
        scale = lax.rsqrt(lax.optimization_barrier(jnp.mean(xf * xf, axis=-1, keepdims=True)) + EPS)
        normed = (xf * scale * norm_gain.astype(jnp.float32)).astype(jnp.bfloat16)
        pre = jnp.dot(normed, w_in, preferred_element_type=jnp.float32)
        hidden = jnp.square(jax.nn.relu(pre)).astype(jnp.bfloat16)
        total = xf
        for index in range(N_TP):
            lower = index * FF_DEV
            partial_sum = jnp.dot(hidden[:, lower:lower + FF_DEV], w_out[lower:lower + FF_DEV, :], preferred_element_type=jnp.float32).astype(jnp.bfloat16)
            partial_sum = lax.optimization_barrier(partial_sum)
            total = total + partial_sum.astype(jnp.float32)
        return total.astype(jnp.bfloat16)
    mixed = lax.map(one_block, pieces)
    return mixed.reshape(TOKENS, D)
```

```python
import jax
import jax.numpy as jnp
from jax import lax
from jax.sharding import PartitionSpec as P

EPS = 1e-06
PLANE = ("grp", "tp")


def local(tokens, norm_gain, w_in, w_out):
    xf = tokens.astype(jnp.float32)
    scale = lax.rsqrt(jnp.mean(xf * xf, axis=-1, keepdims=True) + EPS)
    normed = (xf * scale * norm_gain).astype(jnp.bfloat16)
    group = lax.all_gather(normed, PLANE, axis=0, tiled=True)
    half = w_in.shape[1] // lax.axis_size("grp")
    first = lax.axis_index("grp") * half
    mine_in = lax.dynamic_slice_in_dim(w_in, first, half, 1)
    mine_out = lax.dynamic_slice_in_dim(w_out, first, half, 0)
    pre = jnp.dot(
        group, lax.all_gather(mine_in, "fs", axis=0, tiled=True), preferred_element_type=jnp.float32
    )
    hidden = jnp.square(jax.nn.relu(pre)).astype(jnp.bfloat16)
    terms = jnp.dot(
        hidden, lax.all_gather(mine_out, "fs", axis=1, tiled=True), preferred_element_type=jnp.float32
    )
    summed = lax.psum_scatter(
        terms.astype(jnp.bfloat16), PLANE, scatter_dimension=0, tiled=True
    ).astype(jnp.float32)
    return (xf + summed).astype(jnp.bfloat16)


def solution(mesh):
    in_specs = (P(("grp", "fs", "tp"), None), P(), P("fs", "tp"), P("tp", "fs"))
    out_specs = P(("grp", "fs", "tp"), None)
    return jax.shard_map(local, mesh=mesh, in_specs=in_specs, out_specs=out_specs, check_vma=False)
```

```python
import functools

import jax
import jax.numpy as jnp
from jax import lax
from jax.experimental import pallas as pl
from jax.experimental.pallas import tpu as pltpu
from jax.sharding import PartitionSpec as P

EPS = 1e-06
MESH = pl.DeviceIdType.MESH
CORES = 2
PLANES = 2


def remote(src, dst, send, recv, device):
    pltpu.make_async_remote_copy(
        src_ref=src, dst_ref=dst, send_sem=send, recv_sem=recv, device_id=device, device_id_type=MESH
    ).start()


def done(ref, sem):
    pltpu.make_async_copy(ref, ref, sem).wait()


def kernel(
    Y, n, X, parts, x_ref, g_ref, wi_ref, wo_ref, o_ref,
    norm, wi, wo, hid, crecv, precv, zsend, zrecv, acc,
    tok_send, tok_recv, wi_send, wi_recv, wo_send, wo_recv,
    c_send, c_recv, p_send, p_recv, z_send, z_recv,
):
    y, i, j = lax.axis_index("grp"), lax.axis_index("fs"), lax.axis_index("tp")
    x, core, zp = j // CORES, j % CORES, i % PLANES
    chips = Y * X
    chip = y * X + x
    B, D = x_ref.shape
    HU = wi.shape[1]
    Dr, Dc = wi_ref.shape[0], wo_ref.shape[1]
    W = Dc // parts
    NC = n * parts
    R = norm.shape[0]
    half = R // CORES
    pair_rows = PLANES * B

    partner = (y, i, x * CORES + 1 - core)
    zpair = (y, i + 1 - 2 * zp, j)

    def at_chip(k):
        return (k // X, i, (k % X) * CORES + core)

    def other_chip(o):
        return lax.rem(chip + o, chips)

    direction = jnp.where(i < n // 2, 1, -1)

    barrier = pltpu.get_barrier_semaphore()
    for k in range(1, n):
        pl.semaphore_signal(barrier, inc=1, device_id=(y, lax.rem(i + k, n), j), device_id_type=MESH)
    pl.semaphore_signal(barrier, inc=1, device_id=partner, device_id_type=MESH)
    for o in range(1, chips):
        pl.semaphore_signal(barrier, inc=1, device_id=at_chip(other_chip(o)), device_id_type=MESH)

    def block(c, k, z):
        return (c * chips + k) * PLANES + z

    def rows_of(b):
        return pl.ds(pl.multiple_of(b * B, B), B)

    mine = block(core, chip, zp)

    @pl.loop(0, B // 16)
    def _(r):
        rows = pl.ds(pl.multiple_of(r * 16, 16), 16)
        xf = x_ref[rows, :].astype(jnp.float32)
        scale = lax.rsqrt(jnp.mean(xf * xf, axis=-1, keepdims=True) + EPS)
        out_rows = pl.ds(pl.multiple_of(mine * B + r * 16, 16), 16)
        norm[out_rows, :] = (xf * scale * g_ref[...]).astype(jnp.bfloat16)

    pl.semaphore_wait(barrier, (n - 1) + 1 + (chips - 1))

    count = [0]

    def send_block(b, device):
        ref = norm.at[rows_of(b), :]
        remote(ref, ref, tok_send.at[count[0]], tok_recv.at[b], device)
        count[0] += 1

    send_block(mine, zpair)
    for o in range(1, chips):
        send_block(mine, at_chip(other_chip(o)))
    send_block(mine, partner)

    def in_cols(d):
        return pl.ds(pl.multiple_of(((d % PLANES) * Y + y) * HU, HU), HU)

    def in_rows(s):
        return pl.ds(pl.multiple_of(s * Dr, Dr), Dr)

    def out_cols(cid):
        return pl.ds(pl.multiple_of(cid * W, W), W)

    for k in range(1, n):
        d = lax.rem(i + n - direction * k, n)
        remote(wi_ref.at[:, in_cols(d)], wi.at[in_rows(i), :], wi_send.at[d], wi_recv.at[i], (y, d, j))
    pltpu.make_async_copy(wi_ref.at[:, in_cols(i)], wi.at[in_rows(i), :], wi_recv.at[i]).start()
    for h in range(parts):
        cid = i * parts + h
        for k in range(1, n):
            d = lax.rem(i + n - direction * k, n)
            remote(
                wo_ref.at[in_cols(d), pl.ds(h * W, W)], wo.at[:, out_cols(cid)],
                wo_send.at[d * parts + h], wo_recv.at[cid], (y, d, j),
            )
        pltpu.make_async_copy(
            wo_ref.at[in_cols(i), pl.ds(h * W, W)], wo.at[:, out_cols(cid)], wo_recv.at[cid]
        ).start()

    def arrived(b):
        done(norm.at[rows_of(b), :], tok_recv.at[b])

    paired = block(core, chip, 1 - zp)
    arrived(paired)
    for o in range(1, chips):
        send_block(paired, at_chip(other_chip(o)))
    send_block(paired, partner)
    for z in (zp, 1 - zp):
        for o in range(1, chips):
            b = block(core, other_chip(chips - o), z)
            arrived(b)
            send_block(b, partner)
    for o in range(chips):
        for z in range(PLANES):
            arrived(block(1 - core, other_chip(o), z))

    for s in range(n):
        done(wi.at[in_rows(s), :], wi_recv.at[s])

    TR = min(256, half)

    @pl.loop(0, R // TR)
    def _(r):
        rows = pl.ds(pl.multiple_of(r * TR, TR), TR)
        pre = jnp.dot(norm[rows, :], wi[...], preferred_element_type=jnp.float32)
        hid[rows, :] = jnp.square(jnp.maximum(pre, 0.0)).astype(jnp.bfloat16)

    for q in range(count[0]):
        done(norm.at[rows_of(0), :], tok_send.at[q])

    kept, given = core * half, (1 - core) * half

    def chunk(t):
        s = lax.rem(i + n + direction * (t % n), n)
        return s * parts + t // n

    def multiply(first, cols):
        @pl.loop(0, half // TR)
        def _(r):
            rows = pl.ds(pl.multiple_of(first + r * TR, TR), TR)
            norm[rows, cols] = jnp.dot(
                hid[rows, :], wo[:, cols], preferred_element_type=jnp.float32
            ).astype(jnp.bfloat16)

    def chip_rows(base, k):
        return pl.ds(pl.multiple_of(base + k * pair_rows, pair_rows), pair_rows)

    def fold(k, cols):
        rows = chip_rows(kept, k)
        norm[rows, cols] = (
            norm[rows, cols].astype(jnp.float32) + crecv[chip_rows(0, k), cols].astype(jnp.float32)
        ).astype(jnp.bfloat16)

    @pl.loop(0, NC + 2)
    def _(t):
        @pl.when(t < NC)
        def _():
            cid = chunk(t)
            cols = out_cols(cid)
            done(wo.at[:, cols], wo_recv.at[cid])
            multiply(given, cols)
            remote(
                norm.at[pl.ds(pl.multiple_of(given, half), half), cols], crecv.at[:, cols],
                c_send.at[cid], c_recv.at[cid], partner,
            )
            multiply(kept, cols)
            done(crecv.at[:, cols], c_recv.at[cid])
            for o in range(1, chips):
                k = other_chip(o)
                fold(k, cols)
                remote(
                    norm.at[chip_rows(kept, k), cols], precv.at[chip, :, cols],
                    p_send.at[cid * chips + k], p_recv.at[cid * chips + chip], at_chip(k),
                )
            fold(chip, cols)

        @pl.when(t >= 2)
        def _():
            cid = chunk(t - 2)
            cols = out_cols(cid)
            for o in range(1, chips):
                k = other_chip(o)
                done(precv.at[k, :, cols], p_recv.at[cid * chips + k])

            def total(z):
                inner = pl.ds(pl.multiple_of(z * B, B), B)
                first = kept + chip * pair_rows + z * B
                value = norm[pl.ds(pl.multiple_of(first, B), B), cols].astype(jnp.float32)
                for o in range(1, chips):
                    value += precv[other_chip(o), inner, cols].astype(jnp.float32)
                return value

            zsend[:, cols] = total(1 - zp).astype(jnp.bfloat16)
            remote(zsend.at[:, cols], zrecv.at[:, cols], z_send.at[cid], z_recv.at[cid], zpair)
            acc[:, cols] = total(zp)

    @pl.loop(0, NC)
    def _(t):
        cid = chunk(t)
        cols = out_cols(cid)
        done(zrecv.at[:, cols], z_recv.at[cid])
        total = acc[:, cols] + zrecv[:, cols].astype(jnp.float32)
        o_ref[:, cols] = (x_ref[:, cols].astype(jnp.float32) + total).astype(jnp.bfloat16)

    for k in range(1, n):
        d = lax.rem(i + k, n)
        done(wi.at[in_rows(0), :], wi_send.at[d])
        for h in range(parts):
            done(wo.at[:, out_cols(0)], wo_send.at[d * parts + h])

    @pl.loop(0, NC)
    def _(cid):
        cols = out_cols(cid)
        done(crecv.at[:, cols], c_send.at[cid])
        done(zsend.at[:, cols], z_send.at[cid])
        for o in range(1, chips):
            k = other_chip(o)
            done(precv.at[k, :, cols], p_send.at[cid * chips + k])


def solution(mesh):
    Y, n, T = mesh.shape["grp"], mesh.shape["fs"], mesh.shape["tp"]
    X = T // CORES
    chips = Y * X

    def local(tokens, norm_gain, w_in, w_out):
        B, D = tokens.shape
        HU = w_in.shape[1] // (PLANES * Y)
        Dc = w_out.shape[1]
        parts = 2 if Dc % 256 == 0 else 1
        NC = n * parts
        R = CORES * chips * PLANES * B
        sends = 1 + chips + chips + PLANES * (chips - 1)
        bf16 = jnp.bfloat16
        dma = pltpu.SemaphoreType.DMA
        vmem = pl.BlockSpec(memory_space=pltpu.VMEM)
        hbm = pl.BlockSpec(memory_space=pl.ANY)
        return pl.pallas_call(
            functools.partial(kernel, Y, n, X, parts),
            out_shape=jax.ShapeDtypeStruct((B, D), bf16),
            in_specs=[vmem, vmem, hbm, hbm],
            out_specs=vmem,
            scratch_shapes=[
                pltpu.VMEM((R, D), bf16),
                pltpu.VMEM((D, HU), bf16),
                pltpu.VMEM((HU, D), bf16),
                pltpu.VMEM((R, HU), bf16),
                pltpu.VMEM((R // CORES, D), bf16),
                pltpu.VMEM((chips, PLANES * B, D), bf16),
                pltpu.VMEM((B, D), bf16),
                pltpu.VMEM((B, D), bf16),
                pltpu.VMEM((B, D), jnp.float32),
                dma((sends,)), dma((CORES * chips * PLANES,)),
                dma((n,)), dma((n,)),
                dma((NC,)), dma((NC,)),
                dma((NC,)), dma((NC,)),
                dma((NC * chips,)), dma((NC * chips,)),
                dma((NC,)), dma((NC,)),
            ],
            compiler_params=pltpu.CompilerParams(
                collective_id=0, has_side_effects=True, vmem_limit_bytes=60 * 1024 * 1024
            ),
        )(tokens, norm_gain.reshape(1, D), w_in, w_out)

    in_specs = (P(("grp", "fs", "tp"), None), P(), P("fs", "tp"), P("tp", "fs"))
    out_specs = P(("grp", "fs", "tp"), None)
    return jax.shard_map(local, mesh=mesh, in_specs=in_specs, out_specs=out_specs, check_vma=False)
```

```python
import functools

import jax
import jax.numpy as jnp
from jax import lax
from jax.experimental import pallas as pl
from jax.experimental.pallas import tpu as pltpu
from jax.sharding import PartitionSpec as P

EPS = 1e-06
MESH = pl.DeviceIdType.MESH
CORES = 2
PLANES = 2


def remote(src, dst, send, recv, device):
    pltpu.make_async_remote_copy(
        src_ref=src, dst_ref=dst, send_sem=send, recv_sem=recv, device_id=device, device_id_type=MESH
    ).start()


def done(ref, sem):
    pltpu.make_async_copy(ref, ref, sem).wait()


def kernel(
    Y, n, X, parts, x_ref, g_ref, wi_ref, wo_ref, o_ref,
    norm, wi, wo, hid, crecv, precv, zsend, zrecv, acc,
    tok_send, tok_recv, wi_send, wi_recv, wo_send, wo_recv,
    c_send, c_recv, p_send, p_recv, z_send, z_recv,
):
    y, i, j = lax.axis_index("grp"), lax.axis_index("fs"), lax.axis_index("tp")
    x, core, zp = j // CORES, j % CORES, i % PLANES
    chips = Y * X
    chip = y * X + x
    B, D = x_ref.shape
    HU = wi.shape[1]
    Dr, Dc = wi_ref.shape[0], wo_ref.shape[1]
    W = Dc // parts
    NC = n * parts
    R = norm.shape[0]
    half = R // CORES
    pair_rows = PLANES * B

    partner = (y, i, x * CORES + 1 - core)
    zpair = (y, i + 1 - 2 * zp, j)

    def at_chip(k):
        return (k // X, i, (k % X) * CORES + core)

    def other_chip(o):
        return lax.rem(chip + o, chips)

    direction = jnp.where(i < n // 2, 1, -1)

    barrier = pltpu.get_barrier_semaphore()
    for k in range(1, n):
        pl.semaphore_signal(barrier, inc=1, device_id=(y, lax.rem(i + k, n), j), device_id_type=MESH)
    pl.semaphore_signal(barrier, inc=1, device_id=partner, device_id_type=MESH)
    for o in range(1, chips):
        pl.semaphore_signal(barrier, inc=1, device_id=at_chip(other_chip(o)), device_id_type=MESH)

    def block(c, k, z):
        return (c * chips + k) * PLANES + z

    def rows_of(b):
        return pl.ds(pl.multiple_of(b * B, B), B)

    mine = block(core, chip, zp)

    @pl.loop(0, B // 16)
    def _(r):
        rows = pl.ds(pl.multiple_of(r * 16, 16), 16)
        xf = x_ref[rows, :].astype(jnp.float32)
        scale = lax.rsqrt(jnp.mean(xf * xf, axis=-1, keepdims=True) + EPS)
        out_rows = pl.ds(pl.multiple_of(mine * B + r * 16, 16), 16)
        norm[out_rows, :] = (xf * scale * g_ref[...]).astype(jnp.bfloat16)

    pl.semaphore_wait(barrier, (n - 1) + 1 + (chips - 1))

    count = [0]

    def send_block(b, device):
        ref = norm.at[rows_of(b), :]
        remote(ref, ref, tok_send.at[count[0]], tok_recv.at[b], device)
        count[0] += 1

    send_block(mine, zpair)
    for o in range(1, chips):
        send_block(mine, at_chip(other_chip(o)))
    send_block(mine, partner)

    def in_cols(d):
        return pl.ds(pl.multiple_of(((d % PLANES) * Y + y) * HU, HU), HU)

    def in_rows(s):
        return pl.ds(pl.multiple_of(s * Dr, Dr), Dr)

    def out_cols(cid):
        return pl.ds(pl.multiple_of(cid * W, W), W)

    near = i + 1 - 2 * zp

    def to_planes(send):
        for k in range(1, n):
            d = lax.rem(i + n + direction * k, n)
            pl.when(d != near)(functools.partial(send, d))
        send(near)

    def send_in(d):
        remote(wi_ref.at[:, in_cols(d)], wi.at[in_rows(i), :], wi_send.at[d], wi_recv.at[i], (y, d, j))

    def send_out(h, d):
        cid = i * parts + h
        remote(
            wo_ref.at[in_cols(d), pl.ds(h * W, W)], wo.at[:, out_cols(cid)],
            wo_send.at[d * parts + h], wo_recv.at[cid], (y, d, j),
        )

    to_planes(send_in)
    pltpu.make_async_copy(wi_ref.at[:, in_cols(i)], wi.at[in_rows(i), :], wi_recv.at[i]).start()
    for h in range(parts):
        to_planes(functools.partial(send_out, h))
        cid = i * parts + h
        pltpu.make_async_copy(
            wo_ref.at[in_cols(i), pl.ds(h * W, W)], wo.at[:, out_cols(cid)], wo_recv.at[cid]
        ).start()

    def arrived(b):
        done(norm.at[rows_of(b), :], tok_recv.at[b])

    paired = block(core, chip, 1 - zp)
    arrived(paired)
    for o in range(1, chips):
        send_block(paired, at_chip(other_chip(o)))
    send_block(paired, partner)
    for z in (zp, 1 - zp):
        for o in range(1, chips):
            b = block(core, other_chip(chips - o), z)
            arrived(b)
            send_block(b, partner)
    for o in range(chips):
        for z in range(PLANES):
            arrived(block(1 - core, other_chip(o), z))

    for s in range(n):
        done(wi.at[in_rows(s), :], wi_recv.at[s])

    TR = min(256, half)

    @pl.loop(0, R // TR)
    def _(r):
        rows = pl.ds(pl.multiple_of(r * TR, TR), TR)
        pre = jnp.dot(norm[rows, :], wi[...], preferred_element_type=jnp.float32)
        hid[rows, :] = jnp.square(jnp.maximum(pre, 0.0)).astype(jnp.bfloat16)

    for q in range(count[0]):
        done(norm.at[rows_of(0), :], tok_send.at[q])

    kept, given = core * half, (1 - core) * half

    def chunk(t):
        s = lax.rem(i + n + direction * (t % n), n)
        return s * parts + t // n

    def multiply(first, cols):
        @pl.loop(0, half // TR)
        def _(r):
            rows = pl.ds(pl.multiple_of(first + r * TR, TR), TR)
            norm[rows, cols] = jnp.dot(
                hid[rows, :], wo[:, cols], preferred_element_type=jnp.float32
            ).astype(jnp.bfloat16)

    def chip_rows(base, k):
        return pl.ds(pl.multiple_of(base + k * pair_rows, pair_rows), pair_rows)

    def fold(k, cols):
        rows = chip_rows(kept, k)
        norm[rows, cols] = (
            norm[rows, cols].astype(jnp.float32) + crecv[chip_rows(0, k), cols].astype(jnp.float32)
        ).astype(jnp.bfloat16)

    @pl.loop(0, NC + 2)
    def _(t):
        @pl.when(t < NC)
        def _():
            cid = chunk(t)
            cols = out_cols(cid)
            done(wo.at[:, cols], wo_recv.at[cid])
            multiply(given, cols)
            remote(
                norm.at[pl.ds(pl.multiple_of(given, half), half), cols], crecv.at[:, cols],
                c_send.at[cid], c_recv.at[cid], partner,
            )
            multiply(kept, cols)
            done(crecv.at[:, cols], c_recv.at[cid])
            for o in range(1, chips):
                k = other_chip(o)
                fold(k, cols)
                remote(
                    norm.at[chip_rows(kept, k), cols], precv.at[chip, :, cols],
                    p_send.at[cid * chips + k], p_recv.at[cid * chips + chip], at_chip(k),
                )
            fold(chip, cols)

        @pl.when(t >= 2)
        def _():
            cid = chunk(t - 2)
            cols = out_cols(cid)
            for o in range(1, chips):
                k = other_chip(o)
                done(precv.at[k, :, cols], p_recv.at[cid * chips + k])

            def total(z):
                inner = pl.ds(pl.multiple_of(z * B, B), B)
                first = kept + chip * pair_rows + z * B
                value = norm[pl.ds(pl.multiple_of(first, B), B), cols].astype(jnp.float32)
                for o in range(1, chips):
                    value += precv[other_chip(o), inner, cols].astype(jnp.float32)
                return value

            zsend[:, cols] = total(1 - zp).astype(jnp.bfloat16)
            remote(zsend.at[:, cols], zrecv.at[:, cols], z_send.at[cid], z_recv.at[cid], zpair)
            acc[:, cols] = total(zp)

    @pl.loop(0, NC)
    def _(t):
        cid = chunk(t)
        cols = out_cols(cid)
        done(zrecv.at[:, cols], z_recv.at[cid])
        total = acc[:, cols] + zrecv[:, cols].astype(jnp.float32)
        o_ref[:, cols] = (x_ref[:, cols].astype(jnp.float32) + total).astype(jnp.bfloat16)

    for k in range(1, n):
        d = lax.rem(i + k, n)
        done(wi.at[in_rows(0), :], wi_send.at[d])
        for h in range(parts):
            done(wo.at[:, out_cols(0)], wo_send.at[d * parts + h])

    @pl.loop(0, NC)
    def _(cid):
        cols = out_cols(cid)
        done(crecv.at[:, cols], c_send.at[cid])
        done(zsend.at[:, cols], z_send.at[cid])
        for o in range(1, chips):
            k = other_chip(o)
            done(precv.at[k, :, cols], p_send.at[cid * chips + k])


def solution(mesh):
    Y, n, T = mesh.shape["grp"], mesh.shape["fs"], mesh.shape["tp"]
    X = T // CORES
    chips = Y * X

    def local(tokens, norm_gain, w_in, w_out):
        B, D = tokens.shape
        HU = w_in.shape[1] // (PLANES * Y)
        Dc = w_out.shape[1]
        parts = Dc // 128
        NC = n * parts
        R = CORES * chips * PLANES * B
        sends = 1 + chips + chips + PLANES * (chips - 1)
        bf16 = jnp.bfloat16
        dma = pltpu.SemaphoreType.DMA
        vmem = pl.BlockSpec(memory_space=pltpu.VMEM)
        hbm = pl.BlockSpec(memory_space=pl.ANY)
        return pl.pallas_call(
            functools.partial(kernel, Y, n, X, parts),
            out_shape=jax.ShapeDtypeStruct((B, D), bf16),
            in_specs=[vmem, vmem, hbm, hbm],
            out_specs=vmem,
            scratch_shapes=[
                pltpu.VMEM((R, D), bf16),
                pltpu.VMEM((D, HU), bf16),
                pltpu.VMEM((HU, D), bf16),
                pltpu.VMEM((R, HU), bf16),
                pltpu.VMEM((R // CORES, D), bf16),
                pltpu.VMEM((chips, PLANES * B, D), bf16),
                pltpu.VMEM((B, D), bf16),
                pltpu.VMEM((B, D), bf16),
                pltpu.VMEM((B, D), jnp.float32),
                dma((sends,)), dma((CORES * chips * PLANES,)),
                dma((n,)), dma((n,)),
                dma((NC,)), dma((NC,)),
                dma((NC,)), dma((NC,)),
                dma((NC * chips,)), dma((NC * chips,)),
                dma((NC,)), dma((NC,)),
            ],
            compiler_params=pltpu.CompilerParams(
                collective_id=0, has_side_effects=True, vmem_limit_bytes=60 * 1024 * 1024
            ),
        )(tokens, norm_gain.reshape(1, D), w_in, w_out)

    in_specs = (P(("grp", "fs", "tp"), None), P(), P("fs", "tp"), P("tp", "fs"))
    out_specs = P(("grp", "fs", "tp"), None)
    return jax.shard_map(local, mesh=mesh, in_specs=in_specs, out_specs=out_specs, check_vma=False)
```
